32 devices in a mesh: ep: 4 (over y, x), tp: 8 (over z, core).
Axes of the slice: x: 2, y: 2, z: 4, core: 2. Of those that a mesh axis runs over, the one named last changes fastest.
Arguments:
- mixer_input_channels: bfloat16 [8192, 2048], P('ep', 'tp'), may hold values from -6 to 6
- output_gate_logits: bfloat16 [8192, 2048], P('ep', 'tp'), may hold values from -6 to 6
- head_group_input_map: bfloat16 [8192, 256], P('ep'), may hold values from -6 to 6
- head_group_output_map: bfloat16 [8192, 256], P('ep'), may hold values from -6 to 6
- input_channel_taps: bfloat16 [4, 2048], P(None, 'tp'), may hold values from -3 to 3
- input_map_taps: bfloat16 [4, 256], replicated, may hold values from -3 to 3
- output_map_taps: bfloat16 [4, 256], replicated, may hold values from -3 to 3
- step_logits: float32 [32, 8192], P('tp', 'ep'), may hold values from -5 to 5
- head_log_rate: float32 [32], P('tp'), may hold values from -20 to -2
- extra_log_decay: float32 [32, 8192], P('tp', 'ep'), may hold values from -1 to 0
- head_direct_scale: float32 [32], P('tp'), may hold values from 1 to 6
- gated_norm_scale: bfloat16 [2048], P('tp'), may hold values from 0.099609375 to 1.8984375
- mixer_output_weight: bfloat16 [2048, 2048], P('tp'), may hold values from -0.125 to 0.125
- second_batch_tokens: bfloat16 [1024, 2048], P('ep'), may hold values from -6 to 6
- pre_expert_norm_scale: bfloat16 [2048], replicated, may hold values from 0.099609375 to 1.8984375
- group_router_columns: bfloat16 [2048, 1], replicated
- expert_router_columns: bfloat16 [2048, 4], replicated
- routes: int32 [1024, 2], P('ep'), may hold values from 0 to 3, all different within a row; in each aligned block of 256 rows (0 to 255, 256 to 511, ...) at most 256 rows name the same one
- expert_gate_weight: bfloat16 [4, 2048, 4096], P('ep', None, 'tp'), may hold values from -0.125 to 0.125
- expert_up_weight: bfloat16 [4, 2048, 4096], P('ep', None, 'tp'), may hold values from -0.125 to 0.125
- expert_down_weight: bfloat16 [4, 4096, 2048], P('ep', 'tp'), may hold values from -0.125 to 0.125
Outputs:
- mixer_out: bfloat16 [8192, 2048], P(('ep', 'tp'))
- experts_out: bfloat16 [1024, 2048], P('ep', 'tp')
The draws below stay inside these ranges and needn't reach their ends.
Inputs may be any that keep to these rules, and one draw needn't show every extreme that they name: `routes`: in each aligned block of 256 rows no expert is named more than 256 times, some expert exactly 256 times in some block; a row's two experts differ.
All inputs are finite; a program needn't handle non-finite values.
Results may differ from the reference program's by a relative error of at most 0.019.
Values may be sent and summed in bfloat16 or wider, within the bound.
A program may use at most 128 MiB of HBM per device.

```python
import math
import jax
import jax.numpy as jnp
import numpy as np
from jax import lax

D = 2048
HEADS = 32
HEAD_DIM = 64
STATE = 64
GROUPS = 4
CONV = 4
BLOCK = 128
FF = 4096
TOK_SHARD = 2048
TOKB = 256
INNER = 2048
SEQ = 8192
TOKENS = 1024
EXPERTS = 4
EXPERT_GROUPS = 1
CAP = 256
FF_SHARD = 512
N_EP = 4
N_TP = 8


def draw_step_logits(key, part):
    first, second = jax.random.split(jax.random.fold_in(key, 11))
    span = max(TOK_SHARD // 2, 1)
    offset = jax.random.uniform(second, (HEADS, SEQ // span), jnp.float32, -1.5, 1.5)
    offset = jnp.repeat(offset, span, axis=1)
    noise = jnp.clip(jax.random.normal(first, (HEADS, SEQ), jnp.float32), -3.0, 3.0)
    return (noise + offset).astype(jnp.float32)


def draw_head_log_rate(key, part):
    first, second, third = jax.random.split(jax.random.fold_in(key, 12), 3)
    share = 0.5
    quick = jax.random.uniform(first, (HEADS,), jnp.float32) < share
    quick_rate = jax.random.uniform(second, (HEADS,), jnp.float32, math.log(0.02), math.log(0.1))
    slow_rate = jax.random.uniform(third, (HEADS,), jnp.float32, math.log(0.3), math.log(2.3)) - math.log(SEQ)
    return jnp.where(quick, quick_rate, slow_rate).astype(jnp.float32)


def draw_extra_log_decay(key, part):
    first, second = jax.random.split(jax.random.fold_in(key, 13))
    struck = jax.random.uniform(first, (HEADS, SEQ), jnp.float32) < 6.0 / SEQ
    depth = jax.random.uniform(second, (HEADS, SEQ), jnp.float32, math.log(0.5), math.log(0.8))
    return jnp.where(struck, depth, 0.0).astype(jnp.float32)


def router_columns(key, columns):
    first = jax.random.fold_in(key, 0)
    base = jax.random.normal(first, (D, columns), jnp.float32) / math.sqrt(D)
    return base.astype(jnp.bfloat16)


def draw_group_router_columns(key, part):
    return router_columns(jax.random.fold_in(key, 14), EXPERT_GROUPS)


def draw_expert_router_columns(key, part):
    return router_columns(jax.random.fold_in(key, 15), EXPERTS)


def spiked(result, stream_key, source, target, shards_of, factor):
    owner, partner = [(jnp.arange(result.shape[position]) // (result.shape[position] // shards_of)).reshape([-1 if axis == position else 1 for axis in range(result.ndim)]) for position in (source, target)]
    chosen = jax.random.permutation(stream_key, shards_of)[partner]
    strong = (owner == chosen) | (owner == (partner + shards_of // 2) % shards_of)
    return jnp.where(strong, factor * result, result)


def block_levels(stream_key, extent, cuts, low, high):
    def one(axis_at, blocks):
        draws = jax.random.uniform(jax.random.fold_in(jax.random.fold_in(stream_key, 6), axis_at), (blocks,), jnp.float32, low / len(cuts), high / len(cuts))
        return jnp.repeat(jnp.exp(draws), extent[axis_at] // blocks).reshape((-1,) + (1,) * (len(extent) - axis_at - 1))

    gain = one(*cuts[0])
    for cut in cuts[1:]:
        gain = gain * one(*cut)
    return gain


def deal_out(stream_key, own, number, rows, amount, top, bound, skew):
    order = jax.random.permutation(stream_key, amount)
    packed, common = load_shares(amount, rows * top, bound, skew, True), load_shares(amount, rows * top, bound, skew, False)
    places = jnp.arange(amount)

    def named(sizes, turn):
        used = int((sizes > 0).sum())
        fixed = max(1, used // 4)
        moved = fixed + (places - fixed + turn * (used - fixed)) % max(1, amount - fixed)
        return jnp.zeros((amount,), jnp.int32).at[order[jnp.where(places < fixed, places, moved)]].set(jnp.asarray(sizes, jnp.int32))

    sizes = jnp.where(number % 4 == 0, named(packed, number // 4), named(common, number - number // 4 - 1))
    mixed = jax.random.permutation(jax.random.fold_in(own, 3), amount)
    donor, taker = mixed[0:amount // 2 * 2:2], mixed[1:amount // 2 * 2:2]
    margin = jnp.minimum(sizes[donor] - 1, bound - sizes[taker]) // 2
    margin = jnp.where((donor == order[0]) | (taker == order[0]) | (sizes[taker] == 0), 0, jnp.maximum(margin, 0))
    moved = jax.random.randint(jax.random.fold_in(own, 4), (amount // 2,), 0, 1 << 20) % (margin + 1)
    sizes = sizes.at[donor].add(-moved).at[taker].add(moved)
    members = jnp.searchsorted(jnp.cumsum(sizes), jnp.arange(rows * top), side="right").astype(jnp.int32)
    grid = members.reshape(top, rows).T
    grid = grid[jax.random.permutation(jax.random.fold_in(own, 1), rows)]
    turn = jax.random.randint(jax.random.fold_in(own, 2), (rows, 1), 0, top)
    return jnp.take_along_axis(grid, (jnp.arange(top)[None, :] + turn) % top, axis=1)


def load_shares(number_of, total, limit, skew, full):
    loads = [(1 << 20) // math.isqrt(rank ** skew) + 1 for rank in range(1, number_of + 1)]
    largest = limit if full else min(limit, max(-(-total // number_of), total * loads[0] // sum(loads)))
    least = 1 if total - largest >= number_of - 1 else 0
    given, spare = [largest] + [least] * (number_of - 1), total - largest - least * (number_of - 1)
    while spare > 0:
        free = [i for i in range(1, number_of) if given[i] < largest] or [i for i in range(1, number_of) if given[i] < limit]
        whole, left = sum([loads[i] for i in free]), spare
        for i in free:
            more = min(limit - given[i], max(1, left * loads[i] // whole), spare)
            given[i] = given[i] + more
            spare = spare - more
    return np.array(given)


def bell_draw(key, shape, spread, most, cuts=(), kind=jnp.bfloat16):
    entries = jax.random.normal(key, shape, jnp.float32) * spread
    if len(cuts) > 0:
        entries = block_levels(key, shape, cuts, -0.22, 0.18) * entries
    return jnp.clip(entries, min=-most, max=most).astype(kind)


def noise_with(key, extent, deviation, reach, shards, heavy, kind=jnp.bfloat16):
    result = deviation * jax.random.normal(key, extent, jnp.float32)
    if shards:
        result = result * block_levels(key, extent, shards, -0.22, 0.18)
    return jnp.clip(spiked(result, jax.random.fold_in(key, 3), *heavy), -reach, reach).astype(kind)


def setup_inputs(seed: int = 0) -> dict:
    splits = jax.random.split(jax.random.key(seed), 22)
    mixer_input_channels = bell_draw(splits[0], (SEQ, INNER), 1.0, 6.0, ((0, 4), (1, 8)))
    output_gate_logits = bell_draw(splits[1], (SEQ, INNER), 1.0, 6.0, ((0, 4), (1, 8)))
    head_group_input_map = bell_draw(splits[2], (SEQ, GROUPS * STATE), 1.0, 6.0, ((0, 4),))
    head_group_output_map = bell_draw(splits[3], (SEQ, GROUPS * STATE), 1.0, 6.0, ((0, 4),))
    input_channel_taps = bell_draw(splits[4], (CONV, INNER), CONV ** -0.5, 3.0, ((1, 8),))
    input_map_taps = bell_draw(splits[5], (CONV, GROUPS * STATE), CONV ** -0.5, 3.0)
    output_map_taps = bell_draw(splits[6], (CONV, GROUPS * STATE), CONV ** -0.5, 3.0)
    step_logits = draw_step_logits(jax.random.fold_in(splits[21], 71), 0)
    head_log_rate = draw_head_log_rate(jax.random.fold_in(splits[21], 71), 0)
    extra_log_decay = draw_extra_log_decay(jax.random.fold_in(splits[21], 71), 0)
    head_direct_scale = jnp.clip(1.0 + 5.0 * jax.random.uniform(splits[10], (HEADS,), jnp.float32) ** block_levels(splits[10], (HEADS,), ((0, 8),), -0.2, 0.2), 1.0, 6.0)
    gated_norm_scale = jnp.clip(1.0 + 0.18 * jax.random.normal(splits[11], (INNER,), jnp.float32), 0.099609375, 1.8984375).astype(jnp.bfloat16)
    mixer_output_weight = bell_draw(splits[12], (INNER, D), INNER ** -0.5, 0.125, ((0, 8),))
    second_batch_tokens = bell_draw(splits[13], (TOKENS, D), 1.0, 6.0, ((0, 4),))
    pre_expert_norm_scale = jnp.clip(1.0 + 0.18 * jax.random.normal(splits[14], (D,), jnp.float32), 0.099609375, 1.8984375).astype(jnp.bfloat16)
    group_router_columns = draw_group_router_columns(jax.random.fold_in(splits[21], 71), 0)
    expert_router_columns = draw_expert_router_columns(jax.random.fold_in(splits[21], 71), 0)
    routes_keys = jax.random.split(jax.random.fold_in(splits[17], 1), TOKENS // TOKB)
    routes_turns = jax.random.permutation(jax.random.fold_in(splits[17], 3), TOKENS // TOKB)
    routes = jax.vmap(lambda own, number: deal_out(jax.random.fold_in(splits[17], 2), own, number, TOKB, EXPERTS, 2, CAP, 2))(routes_keys, routes_turns).reshape((TOKENS, 2))
    expert_gate_weight = bell_draw(splits[18], (EXPERTS, D, FF), D ** -0.5, 0.125, ((0, 4), (2, 8)))
    expert_up_weight = bell_draw(splits[19], (EXPERTS, D, FF), D ** -0.5, 0.125, ((0, 4), (2, 8)))
    expert_down_weight = noise_with(splits[20], (EXPERTS, FF, D), FF ** -0.5, 0.125, ((0, 4), (1, 8)), (1, 2, 8, 2.0))
    return {"mixer_input_channels": mixer_input_channels, "output_gate_logits": output_gate_logits, "head_group_input_map": head_group_input_map, "head_group_output_map": head_group_output_map, "input_channel_taps": input_channel_taps, "input_map_taps": input_map_taps, "output_map_taps": output_map_taps, "step_logits": step_logits, "head_log_rate": head_log_rate, "extra_log_decay": extra_log_decay, "head_direct_scale": head_direct_scale, "gated_norm_scale": gated_norm_scale, "mixer_output_weight": mixer_output_weight, "second_batch_tokens": second_batch_tokens, "pre_expert_norm_scale": pre_expert_norm_scale, "group_router_columns": group_router_columns, "expert_router_columns": expert_router_columns, "routes": routes, "expert_gate_weight": expert_gate_weight, "expert_up_weight": expert_up_weight, "expert_down_weight": expert_down_weight}


eps = 1e-06
exact_prec = lax.Precision.HIGHEST

def causal_conv(joined, taps):
    width = taps.shape[0]
    length = joined.shape[0]
    padded = jnp.pad(joined.astype(jnp.float32), ((width - 1, 0), (0, 0)))
    total = jnp.zeros((length, joined.shape[1]), jnp.float32)
    for j in range(width):
        total = total + taps[j].astype(jnp.float32) * padded[j:j + length]
    return jax.nn.silu(total).astype(jnp.bfloat16)

def slot_positions(route_rows, n_experts):
    flat = route_rows.reshape(-1)
    onehot = (flat[:, None] == jnp.arange(n_experts, dtype=jnp.int32)[None, :]).astype(jnp.int32)
    return (lax.optimization_barrier(jnp.sum(onehot * jnp.cumsum(onehot, axis=0), axis=1)) - 1).astype(jnp.int32)

def route_weights(group_logits, expert_logits, routes):
    n_groups = group_logits.shape[1]
    n_experts = expert_logits.shape[1]
    per_group = n_experts // n_groups
    group_lp = jax.nn.log_softmax(group_logits, axis=-1)
    inner_lp = jax.nn.log_softmax(expert_logits.reshape(-1, n_groups, per_group), axis=-1).reshape(-1, n_experts)
    total = jnp.repeat(group_lp, per_group, axis=1) + inner_lp
    pick = routes[:, :, None] == jnp.arange(n_experts, dtype=jnp.int32)[None, None, :]
    chosen = lax.optimization_barrier(jnp.sum(jnp.where(pick, total[:, None, :], 0.0), axis=-1))
    return jax.nn.softmax(chosen, axis=-1)

def expert_apply(items):
    rows, gate_w, up_w, down_w = items
    gate = jnp.dot(rows, gate_w, preferred_element_type=jnp.float32)
    upper = jnp.dot(rows, up_w, preferred_element_type=jnp.float32)
    hidden = (jax.nn.silu(gate) * upper).astype(jnp.bfloat16)
    parts = hidden.reshape(rows.shape[0], N_TP, FF_SHARD).astype(jnp.float32)
    down_parts = down_w.reshape(N_TP, FF_SHARD, D).astype(jnp.float32)
    partial_sums = jnp.einsum('rjf,jfd->jrd', parts, down_parts).astype(jnp.bfloat16)
    return lax.optimization_barrier(jnp.sum(partial_sums.astype(jnp.float32), axis=0)).astype(jnp.bfloat16)

def reference(mixer_input_channels, output_gate_logits, head_group_input_map, head_group_output_map, input_channel_taps, input_map_taps, output_map_taps, step_logits, head_log_rate, extra_log_decay, head_direct_scale, gated_norm_scale, mixer_output_weight, second_batch_tokens, pre_expert_norm_scale, group_router_columns, expert_router_columns, routes, expert_gate_weight, expert_up_weight, expert_down_weight):
    joined = jnp.concatenate([mixer_input_channels, head_group_input_map, head_group_output_map], axis=1)
    taps = jnp.concatenate([input_channel_taps, input_map_taps, output_map_taps], axis=1)
    conv = causal_conv(joined, taps)
    xs = conv[:, :INNER]
    bs = conv[:, INNER:INNER + GROUPS * STATE]
    cs = conv[:, INNER + GROUPS * STATE:]
    time_step = jax.nn.softplus(step_logits)
    position_log_decay = extra_log_decay - time_step * jnp.exp(head_log_rate)[:, None]
    per_group = HEADS // GROUPS
    xs_f = xs.astype(jnp.float32).reshape(SEQ, HEADS, HEAD_DIM)
    x_dt = xs_f * jnp.transpose(time_step)[:, :, None]
    bs_h = jnp.repeat(bs.astype(jnp.float32).reshape(SEQ, GROUPS, STATE), per_group, axis=1)
    cs_h = jnp.repeat(cs.astype(jnp.float32).reshape(SEQ, GROUPS, STATE), per_group, axis=1)
    nblk = SEQ // BLOCK
    items = (x_dt.reshape(nblk, BLOCK, HEADS, HEAD_DIM), bs_h.reshape(nblk, BLOCK, HEADS, STATE), cs_h.reshape(nblk, BLOCK, HEADS, STATE), jnp.transpose(position_log_decay).reshape(nblk, BLOCK, HEADS))
    lower = jnp.tril(jnp.ones((BLOCK, BLOCK), bool))[:, :, None]

    def one_block(state, item):
        xb, bb, cb, lb = item
        cum = jnp.cumsum(lb, axis=0)
        diff = cum[:, None, :] - cum[None, :, :]
        weight = jnp.where(lower, jnp.exp(jnp.where(lower, diff, 0.0)), 0.0)
        scores = jnp.einsum('lhn,shn->lsh', cb, bb, precision=exact_prec)
        inner = jnp.einsum('lsh,shp->lhp', scores * weight, xb, precision=exact_prec)
        carried = jnp.einsum('lhn,hpn->lhp', cb, state, precision=exact_prec) * jnp.exp(cum)[:, :, None]
        tail = jnp.exp(cum[-1:] - cum)
        new_state = state * jnp.exp(cum[-1])[:, None, None] + jnp.einsum('shp,shn->hpn', xb * tail[:, :, None], bb, precision=exact_prec)
        return (new_state, inner + carried)
    start = jnp.zeros((HEADS, HEAD_DIM, STATE), jnp.float32)
    _, ssm = lax.scan(one_block, start, items)
    ssm = ssm.reshape(SEQ, HEADS, HEAD_DIM)
    gated = (ssm + head_direct_scale[None, :, None] * xs_f) * jax.nn.silu(output_gate_logits.astype(jnp.float32)).reshape(SEQ, HEADS, HEAD_DIM)
    gated = gated * lax.rsqrt(lax.optimization_barrier(jnp.mean(gated * gated, axis=-1, keepdims=True)) + eps)
    mixed = (gated.reshape(SEQ, INNER) * gated_norm_scale.astype(jnp.float32)).astype(jnp.bfloat16)
    mixer_out = jnp.dot(mixed, mixer_output_weight, preferred_element_type=jnp.float32).astype(jnp.bfloat16)
    tokens_f = second_batch_tokens.astype(jnp.float32)
    normed = (tokens_f * lax.rsqrt(lax.optimization_barrier(jnp.mean(tokens_f * tokens_f, axis=-1, keepdims=True)) + eps) * pre_expert_norm_scale.astype(jnp.float32)).astype(jnp.bfloat16)
    group_logits = jnp.dot(normed, group_router_columns, preferred_element_type=jnp.float32)
    expert_logits = jnp.dot(normed, expert_router_columns, preferred_element_type=jnp.float32)
    weights = route_weights(group_logits, expert_logits, routes)
    block_routes = routes.reshape(N_EP, TOKB, 2)
    positions = jax.vmap(lambda rows: slot_positions(rows, EXPERTS))(block_routes)
    slots = (block_routes.reshape(N_EP, TOKB * 2) * CAP + positions).astype(jnp.int32)
    token_ids = jnp.repeat(jnp.arange(TOKB, dtype=jnp.int32), 2)
    source = jnp.full((N_EP, EXPERTS * CAP), TOKB, jnp.int32)
    source = jax.vmap(lambda row, slot: row.at[slot].set(token_ids))(source, slots)
    padded = jnp.concatenate([normed.reshape(N_EP, TOKB, D), jnp.zeros((N_EP, 1, D), jnp.bfloat16)], axis=1)
    dispatched = jax.vmap(lambda rows, index: jnp.take(rows, index, axis=0))(padded, source)
    per_expert = jnp.transpose(dispatched.reshape(N_EP, EXPERTS, CAP, D), (1, 0, 2, 3)).reshape(EXPERTS, N_EP * CAP, D)
    outputs = lax.map(expert_apply, (per_expert, expert_gate_weight, expert_up_weight, expert_down_weight))
    by_source = jnp.transpose(outputs.reshape(EXPERTS, N_EP, CAP, D), (1, 0, 2, 3)).reshape(N_EP, EXPERTS * CAP, D)
    picked = jax.vmap(lambda rows, index: jnp.take(rows, index, axis=0))(by_source, slots).astype(jnp.float32)
    combined = lax.optimization_barrier(jnp.sum(picked.reshape(N_EP, TOKB, 2, D) * weights.reshape(N_EP, TOKB, 2, 1), axis=2))
    experts_out = combined.reshape(TOKENS, D).astype(jnp.bfloat16)
    return (mixer_out, experts_out)
```

```python
import jax
import jax.numpy as jnp
from jax import lax
from jax.sharding import PartitionSpec as P

HEADS = 32
STATE = 64
GROUPS = 4
BLOCK = 128
CORES = 2


eps = 1e-06
exact_prec = lax.Precision.DEFAULT


def from_behind(value, axis, steps):
    count = lax.axis_size(axis)
    first, last = (max(0, -steps), min(count, count - steps))
    return lax.ppermute(value, axis, [(source, source + steps) for source in range(first, last)])


def carried_in(state, decay, axis):
    rows = jnp.broadcast_to(decay[:, None, None], (state.shape[0], 8, state.shape[2]))
    packed = jnp.concatenate([state, rows], axis=1).astype(jnp.bfloat16)
    behind = [from_behind(packed, axis, step) for step in range(1, lax.axis_size(axis))]
    total = jnp.zeros_like(state)
    for one in reversed(behind):
        one = one.astype(jnp.float32)
        total = total * one[:, -1:, :1] + one[:, :-8]
    return total


def ring_shift(value, axis, steps):
    count = lax.axis_size(axis)
    return lax.ppermute(value, axis, [(s, (s + steps) % count) for s in range(count)])


def conv_with_rows(joined, before, taps):
    length = joined.shape[0]
    padded = jnp.concatenate([before, joined], axis=0).astype(jnp.float32)
    total = jnp.zeros(joined.shape, jnp.float32)
    for j in range(taps.shape[0]):
        total = total + taps[j].astype(jnp.float32) * padded[j : j + length]
    return jax.nn.silu(total).astype(jnp.bfloat16)


def route_weights(group_logits, expert_logits, routes):
    n_groups = group_logits.shape[1]
    n_experts = expert_logits.shape[1]
    per_group = n_experts // n_groups
    group_lp = jax.nn.log_softmax(group_logits, axis=-1)
    inner_lp = jax.nn.log_softmax(expert_logits.reshape(-1, n_groups, per_group), axis=-1).reshape(
        -1, n_experts
    )
    total = jnp.repeat(group_lp, per_group, axis=1) + inner_lp
    pick = routes[:, :, None] == jnp.arange(n_experts, dtype=jnp.int32)[None, None, :]
    chosen = jnp.sum(jnp.where(pick, total[:, None, :], 0.0), axis=-1)
    share = jax.nn.softmax(chosen, axis=-1)
    return jnp.sum(jnp.where(pick, share[:, :, None], 0.0), axis=1)


def mixer_half(
    mixer_input_channels,
    output_gate_logits,
    head_group_input_map,
    head_group_output_map,
    input_channel_taps,
    input_map_taps,
    output_map_taps,
    step_logits,
    head_log_rate,
    extra_log_decay,
    head_direct_scale,
    gated_norm_scale,
):
    length, width = mixer_input_channels.shape
    heads_dev = head_direct_scale.shape[0]
    head_dim = width // heads_dev
    group = lax.axis_index("tp") * heads_dev // (HEADS // GROUPS)
    first_col = group * STATE
    b_rows = lax.dynamic_slice_in_dim(head_group_input_map, first_col, STATE, 1)
    c_rows = lax.dynamic_slice_in_dim(head_group_output_map, first_col, STATE, 1)
    b_taps = lax.dynamic_slice_in_dim(input_map_taps, first_col, STATE, 1)
    c_taps = lax.dynamic_slice_in_dim(output_map_taps, first_col, STATE, 1)
    joined = jnp.concatenate([mixer_input_channels, b_rows, c_rows], axis=1)
    taps = jnp.concatenate([input_channel_taps, b_taps, c_taps], axis=1)
    reach = taps.shape[0] - 1
    before = from_behind(joined[length - reach :], "ep", 1)
    conv = conv_with_rows(joined, before, taps)
    nblk = length // BLOCK
    xs_f = conv[:, :width].astype(jnp.float32)
    bs_f = conv[:, width : width + STATE].astype(jnp.float32).reshape(nblk, BLOCK, STATE)
    cs_f = conv[:, width + STATE :].astype(jnp.float32).reshape(nblk, BLOCK, STATE)
    head_step_length = jax.nn.softplus(step_logits)
    position_log_decay = extra_log_decay - head_step_length * jnp.exp(head_log_rate)[:, None]
    cum = jnp.cumsum(position_log_decay.reshape(heads_dev, nblk, BLOCK), axis=2)
    step_blocks = jnp.transpose(head_step_length.reshape(heads_dev, nblk, BLOCK), (1, 2, 0))
    x_dt = xs_f.reshape(nblk, BLOCK, heads_dev, head_dim) * step_blocks[..., None]
    lower = jnp.tril(jnp.ones((BLOCK, BLOCK), bool))
    diff = cum[:, :, :, None] - cum[:, :, None, :]
    weight = jnp.where(lower, jnp.exp(jnp.where(lower, diff, 0.0)), 0.0)
    scores = jnp.einsum("bln,bsn->bls", cs_f, bs_f, precision=exact_prec)
    inner = jnp.einsum("bls,hbls,bshp->blhp", scores, weight, x_dt, precision=exact_prec)
    tail = jnp.exp(cum[:, :, -1:] - cum)
    block_state = jnp.einsum("bsn,hbs,bshp->bhpn", bs_f, tail, x_dt, precision=exact_prec)
    block_log = cum[:, :, -1]
    run_log = jnp.cumsum(block_log, axis=1)
    total_log = run_log[:, -1]
    own_state = jnp.einsum(
        "hb,bhpn->hpn", jnp.exp(total_log[:, None] - run_log), block_state, precision=exact_prec
    )
    own_decay = jnp.exp(total_log)
    entering = carried_in(own_state, own_decay, "ep")
    start_log = run_log - block_log
    earlier = jnp.arange(nblk)[:, None] > jnp.arange(nblk)[None, :]
    gap = start_log[:, :, None] - run_log[:, None, :]
    link = jnp.where(earlier, jnp.exp(jnp.where(earlier, gap, 0.0)), 0.0)
    prev = jnp.einsum("hbc,chpn->bhpn", link, block_state, precision=exact_prec)
    prev = prev + jnp.transpose(jnp.exp(start_log))[:, :, None, None] * entering[None]
    carried = jnp.einsum("bln,bhpn->blhp", cs_f, prev, precision=exact_prec)
    carried = carried * jnp.transpose(jnp.exp(cum), (1, 2, 0))[..., None]
    ssm = (inner + carried).reshape(length, heads_dev, head_dim)
    gated = (
        ssm + head_direct_scale[None, :, None] * xs_f.reshape(length, heads_dev, head_dim)
    ) * jax.nn.silu(output_gate_logits.astype(jnp.float32)).reshape(length, heads_dev, head_dim)
    gated = gated * lax.rsqrt(jnp.mean(gated * gated, axis=-1, keepdims=True) + eps)
    mixed = (gated.reshape(length, width) * gated_norm_scale.astype(jnp.float32)).astype(
        jnp.bfloat16
    )
    return rows_by_owner(mixed)


def project(rows_from, out_weight):
    n_ep = lax.axis_size("ep")
    place = lax.axis_index("ep")
    parts = jnp.einsum("rk,ekn->ern", rows_from, out_weight, preferred_element_type=jnp.float32)
    parts = parts.astype(jnp.bfloat16)
    ordered = [
        lax.dynamic_index_in_dim(parts, lax.rem(place + n_ep - q, n_ep), 0, False)
        for q in range(n_ep)
    ]
    return jnp.concatenate(ordered, axis=1)


def tp_moves():
    n_tp = lax.axis_size("tp")
    moves = []
    for flip in range(CORES):
        for level in range(n_tp // CORES):
            target = [(s // CORES + level) * CORES % n_tp + (s % CORES + flip) % CORES for s in range(n_tp)]
            moves.append((level, flip, target))
    return moves


def rows_by_owner(mixed):
    n_tp = lax.axis_size("tp")
    share = mixed.shape[0] // n_tp
    me = lax.axis_index("tp")
    got = []
    for level, flip, target in tp_moves():
        to = (me // CORES + level) * CORES % n_tp + (me % CORES + flip) % CORES
        piece = lax.dynamic_slice_in_dim(mixed, to * share, share, 0)
        if level or flip:
            piece = lax.ppermute(piece, "tp", list(enumerate(target)))
        got.append(piece)
    return jnp.concatenate(got, axis=1)


def out_weight_parts(weight):
    n_ep = lax.axis_size("ep")
    part = weight.shape[1] // n_ep
    own = lax.dynamic_slice_in_dim(weight, lax.axis_index("ep") * part, part, 1)
    levels = [
        lax.ppermute(own, "tp", list(enumerate(target))) if level else own
        for level, flip, target in tp_moves()
        if not flip
    ]
    column = jnp.concatenate(levels, axis=0)
    here = jnp.stack([column] + [ring_shift(column, "ep", k) for k in range(1, n_ep)])
    there = lax.ppermute(here, "tp", list(enumerate(s ^ 1 for s in range(lax.axis_size("tp")))))
    return jnp.concatenate([here, there], axis=1)


def expert_half(
    second_batch_tokens,
    pre_expert_norm_scale,
    group_router_columns,
    expert_router_columns,
    routes,
    expert_gate_weight,
    expert_up_weight,
    expert_down_weight,
):
    n_ep, n_tp = lax.axis_size("ep"), lax.axis_size("tp")
    n_tok, width = second_batch_tokens.shape
    n_experts = expert_router_columns.shape[1]
    cores = CORES
    share = n_tok // cores
    core = lax.axis_index("tp") % cores
    first = core * share
    tokens_f = lax.dynamic_slice_in_dim(second_batch_tokens, first, share, 0).astype(jnp.float32)
    own_routes = lax.dynamic_slice_in_dim(routes, first, share, 0)
    normed = (
        tokens_f
        * lax.rsqrt(jnp.mean(tokens_f * tokens_f, axis=-1, keepdims=True) + eps)
        * pre_expert_norm_scale.astype(jnp.float32)
    ).astype(jnp.bfloat16)
    group_logits = jnp.dot(normed, group_router_columns, preferred_element_type=jnp.float32)
    expert_logits = jnp.dot(normed, expert_router_columns, preferred_element_type=jnp.float32)
    weights = route_weights(group_logits, expert_logits, own_routes)
    coarse = lax.reduce_precision(weights, 8, 7)
    extra = jnp.concatenate([coarse, weights - coarse], axis=1).astype(jnp.bfloat16)
    extra = jnp.pad(extra, ((0, 0), (0, -extra.shape[1] % 128)))
    own = jnp.concatenate([normed, extra], axis=1)
    here = jnp.concatenate([own] + [ring_shift(own, "ep", k) for k in range(1, n_ep)], axis=0)
    there = lax.ppermute(here, "tp", [(s, s ^ 1) for s in range(n_tp)])
    low = jnp.where(core == 0, here, there)
    high = jnp.where(core == 0, there, here)
    rows = jnp.concatenate([low, high], axis=0)
    expert = lax.axis_index("ep")
    pair = rows[:, width : width + 2 * n_experts].astype(jnp.float32)
    wanted = jnp.arange(2 * n_experts) % n_experts == expert
    weight = jnp.sum(jnp.where(wanted, pair, 0.0), axis=1, keepdims=True)
    rows = rows[:, :width]
    gate = jnp.dot(rows, expert_gate_weight[0], preferred_element_type=jnp.float32)
    upper = jnp.dot(rows, expert_up_weight[0], preferred_element_type=jnp.float32)
    hidden = (jax.nn.silu(gate) * upper).astype(jnp.bfloat16)
    down = expert_down_weight[0]
    partial_sums = lax.dot_general(
        down, hidden, (((0,), (1,)), ((), ())), preferred_element_type=jnp.float32
    )
    partial_sums = (partial_sums * weight[:, 0][None, :]).astype(jnp.bfloat16)
    summed = lax.psum_scatter(partial_sums, "tp", scatter_dimension=0, tiled=True)
    blocks = summed.reshape(summed.shape[0], cores, n_ep, share)
    total = blocks[:, :, 0].astype(jnp.float32)
    for k in range(1, n_ep):
        total = total + ring_shift(blocks[:, :, k], "ep", -k).astype(jnp.float32)
    combined = total.reshape(summed.shape[0], n_tok)
    return jnp.transpose(combined).astype(jnp.bfloat16)


def per_device(
    mixer_input_channels,
    output_gate_logits,
    head_group_input_map,
    head_group_output_map,
    input_channel_taps,
    input_map_taps,
    output_map_taps,
    step_logits,
    head_log_rate,
    extra_log_decay,
    head_direct_scale,
    gated_norm_scale,
    mixer_output_weight,
    second_batch_tokens,
    pre_expert_norm_scale,
    group_router_columns,
    expert_router_columns,
    routes,
    expert_gate_weight,
    expert_up_weight,
    expert_down_weight,
):
    out_weight = out_weight_parts(mixer_output_weight)
    rows_from = mixer_half(
        mixer_input_channels,
        output_gate_logits,
        head_group_input_map,
        head_group_output_map,
        input_channel_taps,
        input_map_taps,
        output_map_taps,
        step_logits,
        head_log_rate,
        extra_log_decay,
        head_direct_scale,
        gated_norm_scale,
    )
    experts_out = expert_half(
        second_batch_tokens,
        pre_expert_norm_scale,
        group_router_columns,
        expert_router_columns,
        routes,
        expert_gate_weight,
        expert_up_weight,
        expert_down_weight,
    )
    rows_from, experts_out = lax.optimization_barrier((rows_from, experts_out))
    return (project(rows_from, out_weight), experts_out)


def solution(mesh):
    in_specs = (
        P("ep", "tp"),
        P("ep", "tp"),
        P("ep", None),
        P("ep", None),
        P(None, "tp"),
        P(),
        P(),
        P("tp", "ep"),
        P("tp"),
        P("tp", "ep"),
        P("tp"),
        P("tp"),
        P("tp", None),
        P("ep", None),
        P(),
        P(),
        P(),
        P("ep", None),
        P("ep", None, "tp"),
        P("ep", None, "tp"),
        P("ep", "tp", None),
    )
    out_specs = (P(("ep", "tp"), None), P("ep", "tp"))
    return jax.shard_map(
        per_device, mesh=mesh, in_specs=in_specs, out_specs=out_specs, check_vma=False
    )
```
